32 devices in a mesh: ep: 8 (over z, core), tp: 4 (over y, x).
Axes of the slice: x: 2, y: 2, z: 4, core: 2. Of those that a mesh axis runs over, the one named last changes fastest.
Arguments:
- gate_out: bfloat16 [2048, 1024], P('ep', 'tp'), may hold values from -6 to 6
- gate_in: bfloat16 [2048, 1024], P('ep', 'tp'), may hold values from -6 to 6
- conv_values: bfloat16 [2048, 1024], P('ep', 'tp'), may hold values from -6 to 6
- conv_taps: float32 [3, 1024], P(None, 'tp'), may hold values from -3 to 3
- mixer_proj: bfloat16 [1024, 2048], P('tp'), may hold values from -0.25 to 0.25
- expert_in: bfloat16 [2048, 2048], P('ep'), may hold values from -6 to 6
- norm_gain: float32 [2048], replicated, may hold values from 0.1 to 1.9
- route_ids: int32 [2048, 2], P('ep'), may hold values from 0 to 7, all different within a row; in each aligned block of 256 rows (0 to 255, 256 to 511, ...) at most 86 rows name the same one
- route_scores: float32 [2048, 2], P('ep'), may hold values from 0.1 to 1
- gate_proj: bfloat16 [8, 2048, 4096], P('ep', None, 'tp'), may hold values from -0.125 to 0.125
- up_proj: bfloat16 [8, 2048, 4096], P('ep', None, 'tp'), may hold values from -0.125 to 0.125
- down_proj: bfloat16 [8, 4096, 2048], P('ep', 'tp'), may hold values from -0.125 to 0.125
Outputs:
- mixed: bfloat16 [2048, 2048], P('ep', 'tp')
- expert_mix: bfloat16 [2048, 2048], P('ep', 'tp')
The draws below stay inside these ranges and needn't reach their ends.
Inputs may be any that keep to these rules, and one draw needn't show every extreme that they name: `route_ids`: each row names 2 different experts. Within each aligned block of 256 rows (the rows of one device of ep) no expert is named by more than 86 rows, and in some block an expert is named by exactly 86 rows.
All inputs are finite; a program needn't handle non-finite values.
Results may differ from the reference program's by a relative error of at most 0.015.
Values may be sent and summed in bfloat16 or wider, within the bound.
A program may use at most 64 MiB of HBM per device.

```python
import math
from functools import partial
import jax
import jax.numpy as jnp
import numpy as np
from jax import lax

D = 2048
CW = 1024
FF = 4096
KCONV = 3
TOPK = 2
TOKB_EP = 256
EXPERTS = 8
CAP = 86
TOKA = 2048
TOKB = 2048
N_EP = 8
N_TP = 4


def with_spikes(values, rng, source, target, parts, factor):
    owner, partner = [(jnp.arange(values.shape[position]) // (values.shape[position] // parts)).reshape([-1 if axis == position else 1 for axis in range(values.ndim)]) for position in (source, target)]
    chosen = jax.random.permutation(rng, parts)[partner]
    strong = (owner == chosen) | (owner == (partner + parts // 2) % parts)
    return jnp.where(strong, factor * values, values)


def block_scale(key, extent, shards, low, largest):
    gain, own = 1.0, jax.random.fold_in(key, 6)
    for position, parts in shards:
        draws = jnp.exp(jax.random.uniform(jax.random.fold_in(own, position), (parts,), jnp.float32, low / len(shards), largest / len(shards)))
        gain = gain * jnp.repeat(draws, extent[position] // parts).reshape([-1 if axis == position else 1 for axis in range(len(extent))])
    return gain


def deal_out(own_key, own, number, rows, amount, top, bound, skew):
    sequence = jax.random.permutation(own_key, amount)
    heavy_load, usual = shares(amount, rows * top, bound, skew, True), shares(amount, rows * top, bound, skew, False)
    places = jnp.arange(amount)

    def named(tallies, rotation):
        used = int((tallies > 0).sum())
        fixed = max(1, used // 4)
        moved = fixed + (places - fixed + rotation * (used - fixed)) % max(1, amount - fixed)
        return jnp.zeros((amount,), jnp.int32).at[sequence[jnp.where(places < fixed, places, moved)]].set(jnp.asarray(tallies, jnp.int32))

    tallies = jnp.where(number % 4 == 0, named(heavy_load, number // 4), named(usual, number - number // 4 - 1))
    mixed = jax.random.permutation(jax.random.fold_in(own, 3), amount)
    giver, taker = mixed[0:amount // 2 * 2:2], mixed[1:amount // 2 * 2:2]
    room = jnp.minimum(tallies[giver] - 1, bound - tallies[taker]) // 2
    room = jnp.where((giver == sequence[0]) | (taker == sequence[0]) | (tallies[taker] == 0), 0, jnp.maximum(room, 0))
    moved = jax.random.randint(jax.random.fold_in(own, 4), (amount // 2,), 0, 1 << 20) % (room + 1)
    tallies = tallies.at[giver].add(-moved).at[taker].add(moved)
    items = jnp.searchsorted(jnp.cumsum(tallies), jnp.arange(rows * top), side="right").astype(jnp.int32)
    grid = items.reshape(top, rows).T
    grid = grid[jax.random.permutation(jax.random.fold_in(own, 1), rows)]
    rotation = jax.random.randint(jax.random.fold_in(own, 2), (rows, 1), 0, top)
    return jnp.take_along_axis(grid, (jnp.arange(top)[None, :] + rotation) % top, axis=1)


def shares(count, total, reach, skew, full):
    weights = [(1 << 20) // math.isqrt(standing ** skew) + 1 for standing in range(1, count + 1)]
    largest = reach if full else min(reach, max(-(-total // count), total * weights[0] // sum(weights)))
    least = 1 if total - largest >= count - 1 else 0
    holding, rest = [largest] + [least] * (count - 1), total - largest - least * (count - 1)
    while rest > 0:
        free = [i for i in range(1, count) if holding[i] < largest] or [i for i in range(1, count) if holding[i] < reach]
        pool, budget = sum([weights[i] for i in free]), rest
        for i in free:
            extra = min(reach - holding[i], max(1, budget * weights[i] // pool), rest)
            holding[i] = holding[i] + extra
            rest = rest - extra
    return np.array(holding)


def centred(rng, dims, width, most, shards=(), held_as=jnp.bfloat16):
    drawn = width * jax.random.normal(rng, dims, jnp.float32)
    if shards:
        drawn = drawn * block_scale(rng, dims, shards, -0.22, 0.18)
    return jnp.clip(drawn, -most, most).astype(held_as)


def noise_with(key, extent, scale, limit, pieces, heavy, held_as=jnp.bfloat16):
    drawn = scale * jax.random.normal(key, extent, jnp.float32)
    if pieces:
        drawn = drawn * block_scale(key, extent, pieces, -0.22, 0.18)
    return jnp.clip(with_spikes(drawn, jax.random.fold_in(key, 3), *heavy), -limit, limit).astype(held_as)


def setup_inputs(seed: int = 0) -> dict:
    arg_keys = jax.random.split(jax.random.key(seed), 13)
    gate_out = centred(arg_keys[0], (TOKA, CW), 1.0, 6.0, ((0, 8), (1, 4)))
    gate_in = centred(arg_keys[1], (TOKA, CW), 1.0, 6.0, ((0, 8), (1, 4)))
    conv_values = centred(arg_keys[2], (TOKA, CW), 1.0, 6.0, ((0, 8), (1, 4)))
    conv_taps = centred(arg_keys[3], (KCONV, CW), 0.6, 3.0, ((1, 4),), jnp.float32)
    mixer_proj = noise_with(arg_keys[4], (CW, D), CW ** -0.5, 0.25, ((0, 4),), (0, 1, 4, 2.0))
    expert_in = centred(arg_keys[5], (TOKB, D), 1.0, 6.0, ((0, 8),))
    norm_gain = jnp.clip(1.0 + 0.18 * jax.random.normal(arg_keys[6], (D,), jnp.float32), 0.1, 1.9)
    route_ids_keys = jax.random.split(jax.random.fold_in(arg_keys[7], 1), TOKB // TOKB_EP)
    route_ids_turns = jax.random.permutation(jax.random.fold_in(arg_keys[7], 3), TOKB // TOKB_EP)
    route_ids = jax.vmap(lambda own, number: deal_out(jax.random.fold_in(arg_keys[7], 2), own, number, TOKB_EP, EXPERTS, TOPK, CAP, 1))(route_ids_keys, route_ids_turns).reshape((TOKB, TOPK))
    route_scores = jnp.clip(0.1 + 0.9 * jax.random.uniform(arg_keys[8], (TOKB, TOPK), jnp.float32) ** block_scale(arg_keys[8], (TOKB, TOPK), ((0, 8),), -0.2, 0.2), 0.1, 1.0)
    gate_proj = centred(arg_keys[9], (EXPERTS, D, FF), D ** -0.5, 0.125, ((0, 8), (2, 4)))
    up_proj = centred(arg_keys[10], (EXPERTS, D, FF), D ** -0.5, 0.125, ((0, 8), (2, 4)))
    down_proj = noise_with(arg_keys[11], (EXPERTS, FF, D), FF ** -0.5, 0.125, ((0, 8), (1, 4)), (1, 2, 4, 2.0))
    return {"gate_out": gate_out, "gate_in": gate_in, "conv_values": conv_values, "conv_taps": conv_taps, "mixer_proj": mixer_proj, "expert_in": expert_in, "norm_gain": norm_gain, "route_ids": route_ids, "route_scores": route_scores, "gate_proj": gate_proj, "up_proj": up_proj, "down_proj": down_proj}


def slot_table(route_ids, experts_total, capacity):
    pairs = route_ids.reshape(-1)
    onehot = (pairs[:, None] == jnp.arange(experts_total, dtype=jnp.int32)[None, :]).astype(jnp.int32)
    before = jnp.cumsum(onehot, axis=0) - onehot
    ranking = lax.optimization_barrier(jnp.sum(before * onehot, axis=1))
    return (pairs * capacity + ranking).astype(jnp.int32).reshape(route_ids.shape)

def block_sum(left, right, blocks):
    row_count = left.shape[0]
    inner_width = left.shape[1] // blocks
    left_blocks = left.reshape(row_count, blocks, inner_width).transpose(1, 0, 2)
    right_blocks = right.reshape(blocks, inner_width, right.shape[1])

    def add_block(running, operands):
        rounded = jnp.dot(operands[0], operands[1], preferred_element_type=jnp.float32).astype(jnp.bfloat16)
        rounded = lax.optimization_barrier(rounded)
        return (running + rounded.astype(jnp.float32), None)
    start_sum = jnp.zeros((row_count, right.shape[1]), jnp.float32)
    running, _ = lax.scan(add_block, start_sum, (left_blocks, right_blocks))
    return running

def pick_rows(table, index):
    return jnp.take(table, index, axis=0)

def run_expert(operands):
    tokens, w_gate, w_up, w_down = operands
    gate_value = jnp.dot(tokens, w_gate, preferred_element_type=jnp.float32)
    up_value = jnp.dot(tokens, w_up, preferred_element_type=jnp.float32)
    hidden = (jax.nn.silu(gate_value) * up_value).astype(jnp.bfloat16)
    return block_sum(hidden, w_down, N_TP).astype(jnp.bfloat16)

def reference(gate_out, gate_in, conv_values, conv_taps, mixer_proj, expert_in, norm_gain, route_ids, route_scores, gate_proj, up_proj, down_proj):
    product = gate_in.astype(jnp.float32) * conv_values.astype(jnp.float32)
    seq_len = product.shape[0]
    padded = jnp.concatenate([jnp.zeros((KCONV - 1, CW), jnp.float32), product], axis=0)
    convolved = conv_taps[0] * padded[0:seq_len]
    for offset in range(1, KCONV):
        convolved = convolved + conv_taps[offset] * padded[offset:offset + seq_len]
    branch = (gate_out.astype(jnp.float32) * convolved).astype(jnp.bfloat16)
    mixed = block_sum(branch, mixer_proj, N_TP).astype(jnp.bfloat16)
    rows_wide = expert_in.astype(jnp.float32)
    scaling = lax.rsqrt(lax.optimization_barrier(jnp.mean(rows_wide * rows_wide, axis=1, keepdims=True)) + 1e-06)
    normed = (rows_wide * scaling * norm_gain).astype(jnp.bfloat16)
    slot_count = EXPERTS * CAP
    route_blocks = route_ids.reshape(N_EP, TOKB_EP, TOPK)
    slots = jax.vmap(partial(slot_table, experts_total=EXPERTS, capacity=CAP))(route_blocks)
    sources = jnp.arange(N_EP, dtype=jnp.int32)[:, None, None] * jnp.ones_like(slots)
    token_index = jnp.arange(TOKB_EP, dtype=jnp.int32)[None, :, None] * jnp.ones_like(slots)
    owner = jnp.full((N_EP, slot_count), TOKB_EP, jnp.int32)
    owner = owner.at[sources.reshape(-1), slots.reshape(-1)].set(token_index.reshape(-1))
    normed_blocks = normed.reshape(N_EP, TOKB_EP, D)
    padded_rows = jnp.concatenate([normed_blocks, jnp.zeros((N_EP, 1, D), jnp.bfloat16)], axis=1)
    buffer = jax.vmap(pick_rows)(padded_rows, owner)
    by_expert = buffer.reshape(N_EP, EXPERTS, CAP, D).transpose(1, 0, 2, 3).reshape(EXPERTS, N_EP * CAP, D)
    outputs = lax.map(run_expert, (by_expert, gate_proj, up_proj, down_proj))
    results = outputs.reshape(EXPERTS, N_EP, CAP, D)
    positions = (slots - route_blocks * CAP).astype(jnp.int32)
    picked = results[route_blocks, sources, positions].astype(jnp.float32)
    weights = route_scores / lax.optimization_barrier(jnp.sum(route_scores, axis=1, keepdims=True))
    weights = weights.reshape(N_EP, TOKB_EP, TOPK)
    expert_mix = lax.optimization_barrier(jnp.sum(weights[:, :, :, None] * picked, axis=2)).astype(jnp.bfloat16).reshape(TOKB, D)
    return (mixed, expert_mix)
```

```python
import functools

import jax
import jax.numpy as jnp
from jax import lax
from jax.experimental import pallas as pl
from jax.experimental.pallas import tpu as pltpu
from jax.sharding import PartitionSpec as P

BF16 = jnp.bfloat16
F32 = jnp.float32


def round_up(value, unit):
    return -(-value // unit) * unit


def partner(index, mask):
    bit = 1
    while bit <= mask:
        if mask & bit:
            index = index + bit - 2 * bit * ((index // bit) % 2)
        bit *= 2
    return index


def kernel(
    sizes,
    gate_out,
    gate_in,
    conv_values,
    taps,
    expert_in,
    gain,
    route_ids,
    scores,
    mixer_hbm,
    gate_hbm,
    up_hbm,
    down_hbm,
    mixed,
    expert_mix,
    mixer_w,
    gate_w,
    up_w,
    down_w,
    padded,
    halo,
    product_tail,
    mix_part,
    mix_recv,
    send_rows,
    rows,
    hidden,
    part,
    recv,
    summed,
    back,
    pick,
    weight_sem,
    halo_sem,
    mix_send_sem,
    mix_recv_sem,
    disp_send_sem,
    disp_recv_sem,
    gather_send_sem,
    gather_recv_sem,
    part_send_sem,
    part_recv_sem,
    back_send_sem,
    back_recv_sem,
):
    n_ep, n_tp, slots, width = sizes
    group = 2 if n_ep % 2 == 0 else 1
    while group * slots < 128 and group * 2 <= n_ep:
        group *= 2
    chunks = n_ep // group
    span = group * slots
    ep = lax.axis_index("ep")
    tp = lax.axis_index("tp")
    tokens = expert_in.shape[0]
    model = expert_in.shape[1]
    own = pl.ds(pl.multiple_of(tp * width, width), width)

    def ep_peer(p):
        return {"ep": partner(ep, p)}

    def tp_peer(q):
        return {"tp": partner(tp, q)}

    def remote(src, dst, send, recv, device):
        return pltpu.make_async_remote_copy(
            src_ref=src,
            dst_ref=dst,
            send_sem=send,
            recv_sem=recv,
            device_id=device,
            device_id_type=pl.DeviceIdType.MESH,
        )

    barrier = pltpu.get_barrier_semaphore()
    for p in range(1, n_ep):
        pl.semaphore_signal(barrier, inc=1, device_id=ep_peer(p), device_id_type=pl.DeviceIdType.MESH)
    for q in range(1, n_tp):
        pl.semaphore_signal(barrier, inc=1, device_id=tp_peer(q), device_id_type=pl.DeviceIdType.MESH)

    loads = [
        pltpu.make_async_copy(src, dst, weight_sem.at[i])
        for i, (src, dst) in enumerate(
            [(mixer_hbm, mixer_w), (gate_hbm, gate_w), (up_hbm, up_w), (down_hbm, down_w)]
        )
    ]
    for load in loads:
        load.start()

    ids = route_ids[...]
    lanes = round_up(n_ep, 128)
    expert_iota = lax.broadcasted_iota(jnp.int32, (tokens, lanes), 1)
    named = [(ids[:, k : k + 1] == expert_iota).astype(F32) for k in range(ids.shape[1])]
    counts = functools.reduce(lambda a, b: a + b, named)
    lower = (
        lax.broadcasted_iota(jnp.int32, (tokens, tokens), 0)
        > lax.broadcasted_iota(jnp.int32, (tokens, tokens), 1)
    ).astype(F32)
    before = jnp.dot(lower.astype(BF16), counts.astype(BF16), preferred_element_type=F32)
    slot_iota = lax.broadcasted_iota(jnp.int32, (tokens, n_ep * slots), 1)
    for k in range(ids.shape[1]):
        rank = jnp.sum(before * named[k], axis=1, keepdims=True)
        slot = ids[:, k : k + 1] * slots + rank.astype(jnp.int32)
        pick[k] = (slot_iota == slot).astype(F32).astype(BF16)

    step = 32
    normed_parts = []
    for start in range(0, tokens, step):
        wide = expert_in[start : start + step, :].astype(F32)
        scaling = lax.rsqrt(jnp.mean(wide * wide, axis=1, keepdims=True) + 1e-06)
        block = expert_in[start : start + step, own].astype(F32)
        normed_parts.append((block * scaling * gain[:, own]).astype(BF16))
    normed = jnp.concatenate(normed_parts, axis=0)
    hits = functools.reduce(lambda a, b: a + b, [pick[k] for k in range(ids.shape[1])])
    sent = lax.dot_general(
        hits, normed, (((0,), (0,)), ((), ())), preferred_element_type=F32
    ).astype(BF16)
    for e in range(n_ep):
        send_rows[e] = sent[e * slots : (e + 1) * slots]

    pl.semaphore_wait(barrier, n_ep - 1 + n_tp - 1)

    def position(p):
        return rows.at[pl.ds(p * slots, slots), own]

    dispatches = {
        p: remote(
            send_rows.at[partner(ep, p)],
            position(p),
            disp_send_sem.at[p],
            disp_recv_sem.at[p],
            ep_peer(p),
        )
        for p in range(1, n_ep)
    }
    for p in range(1, n_ep):
        dispatches[p].start()
    rows[0:slots, own] = send_rows[ep]

    seq = gate_in.shape[0]
    tap_count = taps.shape[0]
    edge = halo.shape[0]
    product = gate_in[...].astype(F32) * conv_values[...].astype(F32)
    padded[edge:, :] = product
    product_tail[...] = product[seq - edge :]
    halo_copy = remote(
        product_tail, halo, halo_sem.at[0], halo_sem.at[1], {"ep": (ep + 1) % n_ep}
    )
    halo_copy.start()
    loads[0].wait()
    halo_copy.wait()
    padded[0:edge, :] = halo[...] * (ep > 0).astype(F32)
    convolved = taps[0:1, :] * padded[edge - tap_count + 1 : edge - tap_count + 1 + seq, :]
    for offset in range(1, tap_count):
        base = edge - tap_count + 1 + offset
        convolved = convolved + taps[offset : offset + 1, :] * padded[base : base + seq, :]
    branch = (gate_out[...].astype(F32) * convolved).astype(BF16)
    mix_copies = {}
    for q in list(range(1, n_tp)) + [0]:
        columns = pl.ds(pl.multiple_of(partner(tp, q) * width, width), width)
        mix_part[q] = jnp.dot(branch, mixer_w[:, columns], preferred_element_type=F32).astype(BF16)
        if q:
            mix_copies[q] = remote(
                mix_part.at[q], mix_recv.at[q], mix_send_sem.at[q], mix_recv_sem.at[q], tp_peer(q)
            )
            mix_copies[q].start()

    gathers = {}

    def send_gather(j):
        for p in range(j * group, (j + 1) * group):
            if p:
                dispatches[p].wait_recv()
        block = rows.at[pl.ds(j * span, span), own]
        for q in range(1, n_tp):
            gathers[j, q] = remote(
                block, block, gather_send_sem.at[j, q], gather_recv_sem.at[j, q], tp_peer(q)
            )
            gathers[j, q].start()

    tile = min(256, gate_w.shape[1])
    part_copies = {}
    back_copies = {}

    def run_expert(j):
        for q in range(1, n_tp):
            gathers[j, q].wait_recv()
        here = slice(j * span, (j + 1) * span)

        @pl.loop(0, gate_w.shape[1] // tile)
        def _(i):
            columns = pl.ds(pl.multiple_of(i * tile, tile), tile)
            gate = jnp.dot(rows[here, :], gate_w[:, columns], preferred_element_type=F32)
            up = jnp.dot(rows[here, :], up_w[:, columns], preferred_element_type=F32)
            hidden[:, columns] = (gate / (1.0 + jnp.exp(-gate)) * up).astype(BF16)

        if j == 0:
            loads[3].wait()
        for q in list(range(1, n_tp)) + [0]:
            columns = pl.ds(pl.multiple_of(partner(tp, q) * width, width), width)
            part[j, q] = jnp.dot(hidden[...], down_w[:, columns], preferred_element_type=F32).astype(BF16)
            if q:
                part_copies[j, q] = remote(
                    part.at[j, q],
                    recv.at[j, q],
                    part_send_sem.at[j, q],
                    part_recv_sem.at[j, q],
                    tp_peer(q),
                )
                part_copies[j, q].start()

    def send_back(j):
        total = part[j, 0].astype(F32)
        for q in range(1, n_tp):
            part_copies[j, q].wait_recv()
            total = total + recv[j, q].astype(F32)
        summed[pl.ds(j * span, span), :] = total.astype(BF16)
        for p in range(j * group, (j + 1) * group):
            block = summed.at[pl.ds(p * slots, slots), :]
            if p:
                back_copies[p] = remote(
                    block, back.at[pl.ds(ep * slots, slots), :], back_send_sem.at[p], back_recv_sem.at[p], ep_peer(p)
                )
                back_copies[p].start()
            else:
                back[pl.ds(ep * slots, slots), :] = block[...]

    for j in range(chunks):
        send_gather(j)
        if j == 0:
            loads[1].wait()
            loads[2].wait()
        if j > 0:
            run_expert(j - 1)
        if j > 1:
            send_back(j - 2)
    run_expert(chunks - 1)
    if chunks > 1:
        send_back(chunks - 2)

    total = mix_part[0].astype(F32)
    for q in range(1, n_tp):
        mix_copies[q].wait_recv()
        total = total + mix_recv[q].astype(F32)
    mixed[...] = total.astype(BF16)

    send_back(chunks - 1)

    for p in range(1, n_ep):
        back_copies[p].wait_recv()
    weights = scores[...]
    weights = weights / jnp.sum(weights, axis=1, keepdims=True)
    mix = None
    for k in range(ids.shape[1]):
        picked = jnp.dot(pick[k], back[...], preferred_element_type=F32)
        term = weights[:, k : k + 1] * picked
        mix = term if mix is None else mix + term
    expert_mix[...] = mix.astype(BF16)

    for copies in (dispatches, mix_copies, gathers, part_copies, back_copies):
        for copy in copies.values():
            copy.wait_send()


def shards(
    gate_out,
    gate_in,
    conv_values,
    conv_taps,
    mixer_proj,
    expert_in,
    norm_gain,
    route_ids,
    route_scores,
    gate_proj,
    up_proj,
    down_proj,
):
    n_ep, n_tp = lax.axis_size("ep"), lax.axis_size("tp")
    tokens, model = expert_in.shape
    choices = route_ids.shape[1]
    capacity = max(2, (4 * tokens * choices + 3 * n_ep - 1) // (3 * n_ep))
    slots = round_up(capacity, 16)
    width = model // n_tp
    group = 2 if n_ep % 2 == 0 else 1
    while group * slots < 128 and group * 2 <= n_ep:
        group *= 2
    chunks = n_ep // group
    span = group * slots
    seq, channels = gate_out.shape
    hidden_units = gate_proj.shape[2]
    vmem = pl.BlockSpec(memory_space=pltpu.VMEM)
    hbm = pl.BlockSpec(memory_space=pl.ANY)
    dma = pltpu.SemaphoreType.DMA
    call = pl.pallas_call(
        functools.partial(kernel, (n_ep, n_tp, slots, width)),
        out_shape=(
            jax.ShapeDtypeStruct((seq, width), BF16),
            jax.ShapeDtypeStruct((tokens, width), BF16),
        ),
        in_specs=[vmem] * 8 + [hbm] * 4,
        out_specs=(vmem, vmem),
        scratch_shapes=[
            pltpu.VMEM((channels, model), BF16),
            pltpu.VMEM((model, hidden_units), BF16),
            pltpu.VMEM((model, hidden_units), BF16),
            pltpu.VMEM((hidden_units, model), BF16),
            pltpu.VMEM((seq + 8, channels), F32),
            pltpu.VMEM((8, channels), F32),
            pltpu.VMEM((8, channels), F32),
            pltpu.VMEM((n_tp, seq, width), BF16),
            pltpu.VMEM((n_tp, seq, width), BF16),
            pltpu.VMEM((n_ep, slots, width), BF16),
            pltpu.VMEM((n_ep * slots, model), BF16),
            pltpu.VMEM((span, hidden_units), BF16),
            pltpu.VMEM((chunks, n_tp, span, width), BF16),
            pltpu.VMEM((chunks, n_tp, span, width), BF16),
            pltpu.VMEM((n_ep * slots, width), BF16),
            pltpu.VMEM((n_ep * slots, width), BF16),
            pltpu.VMEM((choices, tokens, n_ep * slots), BF16),
            dma((4,)),
            dma((2,)),
            dma((n_tp,)),
            dma((n_tp,)),
            dma((n_ep,)),
            dma((n_ep,)),
            dma((chunks, n_tp)),
            dma((chunks, n_tp)),
            dma((chunks, n_tp)),
            dma((chunks, n_tp)),
            dma((n_ep,)),
            dma((n_ep,)),
        ],
        compiler_params=pltpu.CompilerParams(
            collective_id=0, has_side_effects=True, vmem_limit_bytes=60 * 1024 * 1024
        ),
    )
    return call(
        gate_out,
        gate_in,
        conv_values,
        conv_taps,
        expert_in,
        norm_gain.reshape(1, model),
        route_ids,
        route_scores,
        mixer_proj,
        gate_proj.reshape(model, hidden_units),
        up_proj.reshape(model, hidden_units),
        down_proj.reshape(hidden_units, model),
    )


def solution(mesh):
    placed = (
        P("ep", "tp"),
        P("ep", "tp"),
        P("ep", "tp"),
        P(None, "tp"),
        P("tp", None),
        P("ep", None),
        P(),
        P("ep", None),
        P("ep", None),
        P("ep", None, "tp"),
        P("ep", None, "tp"),
        P("ep", "tp", None),
    )
    return jax.shard_map(
        shards,
        mesh=mesh,
        in_specs=placed,
        out_specs=(P("ep", "tp"), P("ep", "tp")),
        check_vma=False,
    )
```

```python
import functools

import jax
import jax.numpy as jnp
from jax import lax
from jax.experimental import pallas as pl
from jax.experimental.pallas import tpu as pltpu
from jax.sharding import PartitionSpec as P

BF16 = jnp.bfloat16
F32 = jnp.float32


def round_up(value, unit):
    return -(-value // unit) * unit


def partner(index, mask):
    bit = 1
    while bit <= mask:
        if mask & bit:
            index = index + bit - 2 * bit * ((index // bit) % 2)
        bit *= 2
    return index


def row_steps(n_tp):
    inner = 1
    while inner * inner < n_tp:
        inner *= 2
    return list(range(1, inner)), list(range(inner, n_tp, inner))


def kernel(
    sizes,
    gate_out,
    gate_in,
    conv_values,
    taps,
    expert_in,
    gain,
    route_ids,
    scores,
    mixer_hbm,
    gate_hbm,
    up_hbm,
    down_hbm,
    mixed,
    expert_mix,
    mixer_w,
    gate_w,
    up_w,
    down_w,
    padded,
    halo,
    product_tail,
    mix_part,
    mix_recv,
    send_rows,
    rows,
    hidden,
    part,
    recv,
    summed,
    back,
    pick,
    weight_sem,
    halo_sem,
    mix_send_sem,
    mix_recv_sem,
    disp_send_sem,
    disp_recv_sem,
    gather_send_sem,
    gather_recv_sem,
    part_send_sem,
    part_recv_sem,
    back_send_sem,
    back_recv_sem,
):
    n_ep, n_tp, slots, width = sizes
    group = 2 if n_ep % 2 == 0 else 1
    while group * slots < 128 and group * 2 <= n_ep:
        group *= 2
    chunks = n_ep // group
    span = group * slots
    ep = lax.axis_index("ep")
    tp = lax.axis_index("tp")
    tokens = expert_in.shape[0]
    model = expert_in.shape[1]
    own = pl.ds(pl.multiple_of(tp * width, width), width)

    def ep_peer(p):
        return {"ep": partner(ep, p)}

    def tp_peer(q):
        return {"tp": partner(tp, q)}

    def remote(src, dst, send, recv, device):
        return pltpu.make_async_remote_copy(
            src_ref=src,
            dst_ref=dst,
            send_sem=send,
            recv_sem=recv,
            device_id=device,
            device_id_type=pl.DeviceIdType.MESH,
        )

    barrier = pltpu.get_barrier_semaphore()
    for p in range(1, n_ep):
        pl.semaphore_signal(barrier, inc=1, device_id=ep_peer(p), device_id_type=pl.DeviceIdType.MESH)
    for q in range(1, n_tp):
        pl.semaphore_signal(barrier, inc=1, device_id=tp_peer(q), device_id_type=pl.DeviceIdType.MESH)

    loads = [
        pltpu.make_async_copy(src, dst, weight_sem.at[i])
        for i, (src, dst) in enumerate(
            [(mixer_hbm, mixer_w), (gate_hbm, gate_w), (up_hbm, up_w), (down_hbm, down_w)]
        )
    ]
    for load in loads:
        load.start()

    ids = route_ids[...]
    lanes = round_up(n_ep, 128)
    expert_iota = lax.broadcasted_iota(jnp.int32, (tokens, lanes), 1)
    named = [(ids[:, k : k + 1] == expert_iota).astype(F32) for k in range(ids.shape[1])]
    counts = functools.reduce(lambda a, b: a + b, named)
    lower = (
        lax.broadcasted_iota(jnp.int32, (tokens, tokens), 0)
        > lax.broadcasted_iota(jnp.int32, (tokens, tokens), 1)
    ).astype(F32)
    before = jnp.dot(lower.astype(BF16), counts.astype(BF16), preferred_element_type=F32)
    slot_iota = lax.broadcasted_iota(jnp.int32, (tokens, n_ep * slots), 1)
    for k in range(ids.shape[1]):
        rank = jnp.sum(before * named[k], axis=1, keepdims=True)
        slot = ids[:, k : k + 1] * slots + rank.astype(jnp.int32)
        pick[k] = (slot_iota == slot).astype(F32).astype(BF16)

    step = 32
    normed_parts = []
    for start in range(0, tokens, step):
        wide = expert_in[start : start + step, :].astype(F32)
        scaling = lax.rsqrt(jnp.mean(wide * wide, axis=1, keepdims=True) + 1e-06)
        block = expert_in[start : start + step, own].astype(F32)
        normed_parts.append((block * scaling * gain[:, own]).astype(BF16))
    normed = jnp.concatenate(normed_parts, axis=0)
    hits = functools.reduce(lambda a, b: a + b, [pick[k] for k in range(ids.shape[1])])
    sent = lax.dot_general(
        hits, normed, (((0,), (0,)), ((), ())), preferred_element_type=F32
    ).astype(BF16)
    for e in range(n_ep):
        send_rows[e] = sent[e * slots : (e + 1) * slots]

    pl.semaphore_wait(barrier, n_ep - 1 + n_tp - 1)

    def position(p):
        return rows.at[pl.ds(p * slots, slots), own]

    dispatches = {
        p: remote(
            send_rows.at[partner(ep, p)],
            position(p),
            disp_send_sem.at[p],
            disp_recv_sem.at[p],
            ep_peer(p),
        )
        for p in range(1, n_ep)
    }
    for p in list(range(group, n_ep)) + list(range(1, group)):
        dispatches[p].start()
    rows[0:slots, own] = send_rows[ep]

    seq = gate_in.shape[0]
    tap_count = taps.shape[0]
    edge = halo.shape[0]
    product = gate_in[...].astype(F32) * conv_values[...].astype(F32)
    padded[edge:, :] = product
    product_tail[...] = product[seq - edge :]
    halo_copy = remote(
        product_tail, halo, halo_sem.at[0], halo_sem.at[1], {"ep": (ep + 1) % n_ep}
    )
    halo_copy.start()
    loads[0].wait()
    halo_copy.wait()
    padded[0:edge, :] = halo[...] * (ep > 0).astype(F32)
    convolved = taps[0:1, :] * padded[edge - tap_count + 1 : edge - tap_count + 1 + seq, :]
    for offset in range(1, tap_count):
        base = edge - tap_count + 1 + offset
        convolved = convolved + taps[offset : offset + 1, :] * padded[base : base + seq, :]
    branch = (gate_out[...].astype(F32) * convolved).astype(BF16)
    x_steps, y_steps = row_steps(n_tp)
    halves = ((0, x_steps, y_steps), (1, y_steps, x_steps))

    class ReduceScatter:

        def __init__(self, parts, arrivals, send_sems, recv_sems):
            self.parts, self.arrivals = parts, arrivals
            self.sems = (send_sems, recv_sems)
            self.copies = {}
            self.half = parts.shape[1] // 2

        def cut(self, ref, q, half):
            return ref.at[q, pl.ds(half * self.half, self.half), :]

        def send(self, q, half, to):
            copy = remote(
                self.cut(self.parts, q, half),
                self.cut(self.arrivals, q, half),
                self.sems[0].at[q, half],
                self.sems[1].at[q, half],
                tp_peer(to),
            )
            copy.start()
            self.copies[q, half] = copy

        def first(self, q):
            for half, near, far in halves:
                for step in near:
                    if q - step in [0] + far:
                        self.send(q, half, step)

        def gathered(self, q, half, near):
            total = self.cut(self.parts, q, half)[...].astype(F32)
            for step in near:
                self.copies[step + q, half].wait_recv()
                total = total + self.cut(self.arrivals, step + q, half)[...].astype(F32)
            return total

        def second(self):
            for half, near, far in halves:
                for q in far:
                    total = self.gathered(q, half, near)
                    self.parts[q, half * self.half : (half + 1) * self.half, :] = total.astype(BF16)
                    self.send(q, half, q)

        def finish(self, half):
            _, near, far = halves[half]
            total = self.gathered(0, half, near)
            for q in far:
                self.copies[q, half].wait_recv()
                total = total + self.cut(self.arrivals, q, half)[...].astype(F32)
            return total.astype(BF16)

    order = [q for q in range(n_tp - 1, -1, -1)]

    mix_sum = ReduceScatter(mix_part, mix_recv, mix_send_sem, mix_recv_sem)
    for q in order:
        columns = pl.ds(pl.multiple_of(partner(tp, q) * width, width), width)
        mix_part[q] = jnp.dot(branch, mixer_w[:, columns], preferred_element_type=F32).astype(BF16)
        if q:
            mix_sum.first(q)

    gathers = {}

    def columns_of(q):
        return pl.ds(pl.multiple_of(partner(tp, q) * width, width), width)

    def send_block(j, q, first_row, row_count, half, to):
        block = rows.at[pl.ds(first_row, row_count), columns_of(q)]
        copy = remote(
            block,
            block,
            gather_send_sem.at[j, q ^ to, half],
            gather_recv_sem.at[j, q ^ to, half],
            tp_peer(to),
        )
        copy.start()
        gathers[j, q ^ to, half] = copy

    def send_gather(j):
        for p in range(j * group, (j + 1) * group):
            if p:
                dispatches[p].wait_recv()
        for step in x_steps + y_steps:
            send_block(j, 0, j * span, span, 0, step)

    def forward(j):
        for step in x_steps + y_steps:
            gathers[j, step, 0].wait_recv()
        for half, near, far in halves:
            for via in near:
                for to in far:
                    send_block(j, via, j * span + half * (span // 2), span // 2, half, to)

    tile = min(256, gate_w.shape[1])
    sums = {}
    back_copies = {}

    def run_expert(j, first):
        for (at, q, half), copy in list(gathers.items()):
            if at == j and q not in x_steps + y_steps:
                copy.wait_recv()
        here = slice(j * span, (j + 1) * span)
        if first:
            loads[1].wait()
            loads[2].wait()

        @pl.loop(0, gate_w.shape[1] // tile)
        def _(i):
            columns = pl.ds(pl.multiple_of(i * tile, tile), tile)
            gate = jnp.dot(rows[here, :], gate_w[:, columns], preferred_element_type=F32)
            up = jnp.dot(rows[here, :], up_w[:, columns], preferred_element_type=F32)
            hidden[:, columns] = (gate / (1.0 + jnp.exp(-gate)) * up).astype(BF16)

        if first:
            loads[3].wait()
        sums[j] = ReduceScatter(part.at[j], recv.at[j], part_send_sem.at[j], part_recv_sem.at[j])
        for q in order:
            part[j, q] = jnp.dot(
                hidden[...], down_w[:, columns_of(q)], preferred_element_type=F32
            ).astype(BF16)
            if q:
                sums[j].first(q)

    def send_back(j):
        for half in range(2):
            summed[pl.ds(j * span + half * (span // 2), span // 2), :] = sums[j].finish(half)
        for p in range(j * group, (j + 1) * group):
            block = summed.at[pl.ds(p * slots, slots), :]
            if p:
                back_copies[p] = remote(
                    block,
                    back.at[pl.ds(ep * slots, slots), :],
                    back_send_sem.at[p],
                    back_recv_sem.at[p],
                    ep_peer(p),
                )
                back_copies[p].start()
            else:
                back[pl.ds(ep * slots, slots), :] = block[...]

    turns = list(range(1, chunks)) + [0]
    for i, j in enumerate(turns):
        send_gather(j)
        if i == 0:
            mix_sum.second()
        if i > 0:
            forward(turns[i - 1])
        if i > 1:
            run_expert(turns[i - 2], i == 2)
        if i > 2:
            sums[turns[i - 3]].second()
        if i > 3:
            send_back(turns[i - 4])
    forward(turns[-1])
    for i in range(chunks - 2, chunks):
        run_expert(turns[i], i == 0)
        sums[turns[i - 1]].second()
        if i > 1:
            send_back(turns[i - 2])
    for half in range(2):
        rest = mixed.shape[0] // 2
        mixed[half * rest : (half + 1) * rest, :] = mix_sum.finish(half)
    sums[turns[-1]].second()
    send_back(turns[-2])
    send_back(turns[-1])

    for p in range(1, n_ep):
        back_copies[p].wait_recv()
    weights = scores[...]
    weights = weights / jnp.sum(weights, axis=1, keepdims=True)
    mix = None
    for k in range(ids.shape[1]):
        picked = jnp.dot(pick[k], back[...], preferred_element_type=F32)
        term = weights[:, k : k + 1] * picked
        mix = term if mix is None else mix + term
    expert_mix[...] = mix.astype(BF16)

    started = [dispatches, gathers, back_copies, mix_sum.copies]
    started += [total.copies for total in sums.values()]
    for copies in started:
        for copy in copies.values():
            copy.wait_send()


def shards(
    gate_out,
    gate_in,
    conv_values,
    conv_taps,
    mixer_proj,
    expert_in,
    norm_gain,
    route_ids,
    route_scores,
    gate_proj,
    up_proj,
    down_proj,
):
    n_ep, n_tp = lax.axis_size("ep"), lax.axis_size("tp")
    tokens, model = expert_in.shape
    choices = route_ids.shape[1]
    capacity = max(2, (4 * tokens * choices + 3 * n_ep - 1) // (3 * n_ep))
    slots = round_up(capacity, 16)
    width = model // n_tp
    group = 2 if n_ep % 2 == 0 else 1
    while group * slots < 128 and group * 2 <= n_ep:
        group *= 2
    chunks = n_ep // group
    span = group * slots
    seq, channels = gate_out.shape
    hidden_units = gate_proj.shape[2]
    vmem = pl.BlockSpec(memory_space=pltpu.VMEM)
    hbm = pl.BlockSpec(memory_space=pl.ANY)
    dma = pltpu.SemaphoreType.DMA
    call = pl.pallas_call(
        functools.partial(kernel, (n_ep, n_tp, slots, width)),
        out_shape=(
            jax.ShapeDtypeStruct((seq, width), BF16),
            jax.ShapeDtypeStruct((tokens, width), BF16),
        ),
        in_specs=[vmem] * 8 + [hbm] * 4,
        out_specs=(vmem, vmem),
        scratch_shapes=[
            pltpu.VMEM((channels, model), BF16),
            pltpu.VMEM((model, hidden_units), BF16),
            pltpu.VMEM((model, hidden_units), BF16),
            pltpu.VMEM((hidden_units, model), BF16),
            pltpu.VMEM((seq + 8, channels), F32),
            pltpu.VMEM((8, channels), F32),
            pltpu.VMEM((8, channels), F32),
            pltpu.VMEM((n_tp, seq, width), BF16),
            pltpu.VMEM((n_tp, seq, width), BF16),
            pltpu.VMEM((n_ep, slots, width), BF16),
            pltpu.VMEM((n_ep * slots, model), BF16),
            pltpu.VMEM((span, hidden_units), BF16),
            pltpu.VMEM((chunks, n_tp, span, width), BF16),
            pltpu.VMEM((chunks, n_tp, span, width), BF16),
            pltpu.VMEM((n_ep * slots, width), BF16),
            pltpu.VMEM((n_ep * slots, width), BF16),
            pltpu.VMEM((choices, tokens, n_ep * slots), BF16),
            dma((4,)),
            dma((2,)),
            dma((n_tp, 2)),
            dma((n_tp, 2)),
            dma((n_ep,)),
            dma((n_ep,)),
            dma((chunks, n_tp, 2)),
            dma((chunks, n_tp, 2)),
            dma((chunks, n_tp, 2)),
            dma((chunks, n_tp, 2)),
            dma((n_ep,)),
            dma((n_ep,)),
        ],
        compiler_params=pltpu.CompilerParams(
            collective_id=0, has_side_effects=True, vmem_limit_bytes=60 * 1024 * 1024
        ),
    )
    return call(
        gate_out,
        gate_in,
        conv_values,
        conv_taps,
        expert_in,
        norm_gain.reshape(1, model),
        route_ids,
        route_scores,
        mixer_proj,
        gate_proj.reshape(model, hidden_units),
        up_proj.reshape(model, hidden_units),
        down_proj.reshape(hidden_units, model),
    )


def solution(mesh):
    placed = (
        P("ep", "tp"),
        P("ep", "tp"),
        P("ep", "tp"),
        P(None, "tp"),
        P("tp", None),
        P("ep", None),
        P(),
        P("ep", None),
        P("ep", None),
        P("ep", None, "tp"),
        P("ep", None, "tp"),
        P("ep", "tp", None),
    )
    return jax.shard_map(
        shards,
        mesh=mesh,
        in_specs=placed,
        out_specs=(P("ep", "tp"), P("ep", "tp")),
        check_vma=False,
    )
```
